256 devices in a mesh: kv: 32 (over z, y), tp: 8 (over x, core).
Axes of the slice: x: 4, y: 4, z: 8, core: 2. Of those that a mesh axis runs over, the one named last changes fastest.
Arguments:
- tokens: bfloat16 [32768, 1024], P('kv', 'tp'), may hold values from -6 to 6
- query_weight: bfloat16 [1024, 2048], P(None, 'tp'), may hold values from -0.1875 to 0.1875
- latent_weight: bfloat16 [1024, 128], replicated, may hold values from -0.1875 to 0.1875
- query_gain: float32 [128], replicated, may hold values from 0.5 to 1.5
- key_gain: float32 [128], replicated, may hold values from 0.5 to 1.5
- value_up: bfloat16 [16, 128, 64], P('tp'), may hold values from -0.5 to 0.5
- out_weight: bfloat16 [1024, 1024], P('tp'), may hold values from -0.25 to 0.25
- out_gain: float32 [1024], replicated, may hold values from 0.5 to 1.5
- chosen: int32 [256, 32], P('kv'), may hold values from -1 to 255, as said below
Outputs:
- mixed_out: bfloat16 [32768, 1024], P('kv', 'tp')
The draws below stay inside these ranges and needn't reach their ends.
Inputs may be any that keep to these rules, and one draw needn't show every extreme that they name: Row b lists the key blocks chosen for query block b: entry 0 is b itself, then distinct blocks before b, then -1 in every unused place. Block j is held by index j // 8 of kv. All query blocks of one index of kv together choose at most 2 distinct blocks held by any one other index, and some pair of indices reaches that bound; blocks held by the same index are chosen freely.
All inputs are finite; a program needn't handle non-finite values.
Results may differ from the reference program's by a relative error of at most 0.02.
Values may be sent and summed in bfloat16 or wider, within the bound.
No kernel may reach another device: no remote copies, remote signals or barrier semaphores. Data moves between devices by JAX's collectives and lax.ppermute only.
A program may use at most 64 MiB of HBM per device.

```python
import jax
import jax.numpy as jnp
from jax import lax

D = 1024
HEADS = 16
LATENT = 128
VDIM = 64
BLOCK = 128
PICKS = 32
PER_OWNER = 2
TOKENS = 32768
BLOCKS_DEV = 8
BLOCKS = 256


def draw_chosen(key, part):
    per_dev = BLOCKS_DEV
    block_count = BLOCKS
    devices = block_count // per_dev
    level_key = jax.random.fold_in(key, 11)
    order_key = jax.random.fold_in(key, 12)
    pick_key = jax.random.fold_in(key, 13)
    classes = jax.random.randint(level_key, (devices,), 0, 4)
    levels = jnp.where(classes == 0, PER_OWNER, jnp.where(classes == 1, 1, 0)).astype(jnp.int32)
    levels = jnp.minimum(levels, PER_OWNER)
    levels = levels.at[0].set(PER_OWNER)
    block_ids = jnp.arange(block_count, dtype=jnp.int32)
    owner_ids = block_ids // per_dev
    local_ids = block_ids % per_dev
    raw_order = jax.random.randint(order_key, (devices, block_count), 0, 1 << 16)
    distinct = raw_order * per_dev + local_ids[None, :]
    grouped = distinct.reshape(devices, devices, per_dev)
    ranking = jnp.argsort(jnp.argsort(grouped, axis=2), axis=2).reshape(devices, block_count)
    requester = jnp.arange(devices, dtype=jnp.int32)
    allowed = (ranking < levels[owner_ids][None, :]) & (owner_ids[None, :] < requester[:, None])
    local_before = (owner_ids[None, :] == owner_ids[:, None]) & (block_ids[None, :] < block_ids[:, None])
    candidate = allowed[owner_ids] | local_before
    raw_pick = jax.random.randint(pick_key, (block_count, block_count), 0, 1 << 16)
    scores = jnp.where(candidate, raw_pick * block_count + block_ids[None, :], -1)
    best_scores, where_best = lax.top_k(scores, PICKS - 1)
    others = jnp.where(best_scores >= 0, where_best, -1).astype(jnp.int32)
    return jnp.concatenate([block_ids[:, None], others], axis=1).astype(jnp.int32)


def with_spikes(result, rng, source, target, shards_of, factor):
    def block_of(dim):
        return (jnp.arange(result.shape[dim]) // (result.shape[dim] // shards_of)).reshape((-1,) + (1,) * (result.ndim - 1 - dim))

    one_side = jax.random.permutation(rng, shards_of)[block_of(target)]
    far = (block_of(target) + shards_of // 2) % shards_of
    return jnp.where((block_of(source) == one_side) | (block_of(source) == far), factor * result, result)


def block_scale(stream_key, dims, cuts, smallest, high):
    gain = 1.0
    for position, shards_of in cuts:
        draws = jax.random.uniform(jax.random.fold_in(jax.random.fold_in(stream_key, 6), position), (shards_of,), jnp.float32, smallest / len(cuts), high / len(cuts))
        gain = gain * jnp.repeat(jnp.exp(draws), dims[position] // shards_of).reshape((-1,) + (1,) * (len(dims) - 1 - position))
    return gain


def bell_draw(own_key, dims, width, most, shards=(), kind=jnp.bfloat16):
    array = width * jax.random.normal(own_key, dims, jnp.float32)
    if shards:
        array = array * block_scale(own_key, dims, shards, -0.22, 0.18)
    return jnp.clip(array, -most, most).astype(kind)


def bell_draw_with(key, extent, width, limit, pieces, heavy, kind=jnp.bfloat16):
    drawn = width * jax.random.normal(key, extent, jnp.float32)
    if pieces:
        drawn = drawn * block_scale(key, extent, pieces, -0.22, 0.18)
    return jnp.clip(with_spikes(drawn, jax.random.fold_in(key, 3), *heavy), -limit, limit).astype(kind)


def setup_inputs(seed: int = 0) -> dict:
    splits = jax.random.split(jax.random.key(seed), 10)
    tokens = bell_draw(splits[0], (TOKENS, D), 1.0, 6.0, ((0, 32), (1, 8)))
    query_weight = bell_draw(splits[1], (D, HEADS * LATENT), D ** -0.5, 0.1875, ((1, 8),))
    latent_weight = bell_draw(splits[2], (D, LATENT), D ** -0.5, 0.1875)
    query_gain = jnp.clip(1.0 + 0.1 * jax.random.normal(splits[3], (LATENT,), jnp.float32), 0.5, 1.5)
    key_gain = jnp.clip(1.0 + 0.1 * jax.random.normal(splits[4], (LATENT,), jnp.float32), 0.5, 1.5)
    value_up = bell_draw(splits[5], (HEADS, LATENT, VDIM), LATENT ** -0.5, 0.5, ((0, 8),))
    out_weight = bell_draw_with(splits[6], (HEADS * VDIM, D), (HEADS * VDIM) ** -0.5, 0.25, ((0, 8),), (0, 1, 8, 2.0))
    out_gain = jnp.clip(1.0 + 0.1 * jax.random.normal(splits[7], (D,), jnp.float32), 0.5, 1.5)
    chosen = draw_chosen(jax.random.fold_in(splits[9], 71), 0)
    return {"tokens": tokens, "query_weight": query_weight, "latent_weight": latent_weight, "query_gain": query_gain, "key_gain": key_gain, "value_up": value_up, "out_weight": out_weight, "out_gain": out_gain, "chosen": chosen}


epsilon = 1e-06
masked_score = -1e+30

def rms_scale(values, gain_row):
    widened = values.astype(jnp.float32)
    mean_sq = lax.optimization_barrier(jnp.mean(widened * widened, axis=-1, keepdims=True))
    return (widened * lax.rsqrt(mean_sq + epsilon) * gain_row).astype(jnp.bfloat16)

def reference(tokens, query_weight, latent_weight, query_gain, key_gain, value_up, out_weight, out_gain, chosen):
    queries = jnp.dot(tokens, query_weight, preferred_element_type=jnp.float32).astype(jnp.bfloat16)
    queries = rms_scale(queries.reshape(TOKENS, HEADS, LATENT), query_gain)
    latent = jnp.dot(tokens, latent_weight, preferred_element_type=jnp.float32).astype(jnp.bfloat16)
    normed_keys = rms_scale(latent, key_gain)
    key_blocks = normed_keys.reshape(BLOCKS, BLOCK, LATENT)
    value_blocks = latent.reshape(BLOCKS, BLOCK, LATENT)
    query_blocks = queries.reshape(BLOCKS, BLOCK, HEADS, LATENT)
    offsets = jnp.arange(BLOCK, dtype=jnp.int32)

    def attend(packed):
        query_block, chosen_row, start_pos = packed
        clamped = jnp.maximum(chosen_row, 0).astype(jnp.int32)
        picked_keys = key_blocks[clamped].astype(jnp.float32)
        picked_values = value_blocks[clamped].astype(jnp.float32)
        scores = jnp.einsum('qhl,ckl->qhck', query_block.astype(jnp.float32), picked_keys) * LATENT ** (-0.5)
        key_pos = clamped[:, None] * BLOCK + offsets[None, :]
        query_pos = start_pos + offsets
        allowed = (chosen_row[:, None] >= 0)[None] & (key_pos[None] <= query_pos[:, None, None])
        allowed = allowed[:, None]
        scores = jnp.where(allowed, scores, masked_score)
        row_max = lax.optimization_barrier(jnp.max(scores, axis=(2, 3), keepdims=True))
        exp_scores = jnp.where(allowed, jnp.exp(scores - row_max), 0.0)
        weights = (exp_scores / lax.optimization_barrier(jnp.sum(exp_scores, axis=(2, 3), keepdims=True))).astype(jnp.bfloat16)
        attended = jnp.einsum('qhck,ckl->qhl', weights.astype(jnp.float32), picked_values)
        return attended.astype(jnp.bfloat16)
    block_starts = jnp.arange(BLOCKS, dtype=jnp.int32) * BLOCK
    attended = lax.map(attend, (query_blocks, chosen, block_starts))
    attended = attended.reshape(TOKENS, HEADS, LATENT)
    heads_out = jnp.einsum('thl,hlv->thv', attended.astype(jnp.float32), value_up.astype(jnp.float32))
    heads_out = heads_out.astype(jnp.bfloat16).reshape(TOKENS, HEADS * VDIM)
    projected = jnp.dot(heads_out, out_weight, preferred_element_type=jnp.float32)
    return rms_scale(projected, out_gain)
```

```python
import functools
import math

import jax
import jax.numpy as jnp
from jax import lax
from jax.experimental import pallas as pl
from jax.experimental.pallas import tpu as pltpu
from jax.sharding import Mesh
from jax.sharding import PartitionSpec as P

BLOCK = 128
PER_OWNER = 2
KV = ("kv_0", "kv_1")
TP = ("x", "core")
GROUP = 8


epsilon = 1e-06
f32 = jnp.float32
bf16 = jnp.bfloat16

VMEM = pl.BlockSpec(memory_space=pltpu.VMEM)
SMEM = pl.BlockSpec(memory_space=pltpu.SMEM)


def shifted(part, axis, step):
    n = lax.axis_size(axis)
    return lax.ppermute(part, axis, [(i, (i + step) % n) for i in range(n)])


def gathered(part):
    steps = range(1, lax.axis_size("x"))
    along_x = [part] + [shifted(part, "x", d) for d in steps]
    return along_x + [shifted(p, "core", 1) for p in along_x]


def normed(values, gain_row):
    wide = values.astype(f32)
    mean_sq = jnp.mean(wide * wide, axis=-1, keepdims=True)
    return (wide * lax.rsqrt(mean_sq + epsilon) * gain_row).astype(bf16)


def piece_order(meta, count):
    chips = count // 2
    x, core = meta[0], meta[1]
    from_x = [lax.rem(x - d + chips, chips) for d in range(chips)]
    return [2 * c + core for c in from_x] + [2 * c + 1 - core for c in from_x]


def project_kernel(meta, asked, *refs):
    pieces, (qw, lw, qgain, q_out, lat_out, send_out, wcat) = refs[:-7], refs[-7:]
    n = len(pieces)
    width = pieces[0].shape[1]
    rows = pieces[0].shape[0]
    cols = qw.shape[1]
    lat_width = lw.shape[1]
    heads = cols // lat_width
    for i, p in enumerate(piece_order(meta, n)):
        src = pl.ds(pl.multiple_of(p * width, width), width)
        wcat[i * width : (i + 1) * width, :cols] = qw[src, :]
        wcat[i * width : (i + 1) * width, cols:] = lw[src, :]
    gain = qgain[...]
    step = 2 * BLOCK
    for r in range(0, rows, step):
        lhs = jnp.concatenate([p[r : r + step, :] for p in pieces], axis=1)
        acc = jnp.dot(lhs, wcat[...], preferred_element_type=f32)
        for h in range(heads):
            q = normed(acc[:, h * lat_width : (h + 1) * lat_width].astype(bf16), gain)
            for k in range(step // BLOCK):
                q_out[r // BLOCK + k, h * BLOCK : (h + 1) * BLOCK, :] = q[k * BLOCK : (k + 1) * BLOCK]
        lat = acc[:, cols:].astype(bf16)
        sl = lat_out.shape[1]
        lat_out[r // sl : (r + step) // sl] = lat.reshape(step // sl, sl, lat_width)
    me = 2 * meta[0] + meta[1]
    for o in range(send_out.shape[0]):
        for s in range(PER_OWNER):
            send_out[o, s] = lat_out[asked[o, s] * n + me]


def attend_kernel(table, count, *refs):
    pieces = refs[:-8]
    q_ref, own, kgain, vup, out, keys, vals, acc = refs[-8:]
    blocks = q_ref.shape[0]
    n = len(pieces)
    sl = pieces[0].shape[1]
    slots = pieces[0].shape[0]
    gain = kgain[...]
    ones = jnp.ones((BLOCK, BLOCK), bf16)
    lat_w = own.shape[-1]

    def place(slot, lat):
        keys[slot] = normed(lat, gain)
        vals[slot, :, :lat_w] = lat
        vals[slot, :, lat_w:] = ones

    def place_own(b, _):
        place(b, own[b])
        return 0

    def place_far(s, _):
        place(blocks + s, jnp.concatenate([p[s] for p in pieces], axis=0))
        return 0

    lax.fori_loop(0, blocks, place_own, 0, unroll=2)
    lax.fori_loop(0, slots, place_far, 0, unroll=4)
    keys[blocks + slots] = jnp.zeros((BLOCK, lat_w), bf16)
    vals[blocks + slots] = jnp.zeros((BLOCK, 2 * lat_w), bf16)

    rows = q_ref.shape[1]
    pair = 2
    heads = rows // BLOCK

    def part(q, idx, masked):
        k = jnp.concatenate([keys[i] for i in idx], axis=0)
        s = lax.dot_general(q, k, (((1,), (1,)), ((), ())), preferred_element_type=f32)
        w = jnp.exp2(s)
        if masked:
            at = lax.broadcasted_iota(jnp.int32, s.shape, 1)
            row = lax.broadcasted_iota(jnp.int32, s.shape, 0) & (BLOCK - 1)
            w = jnp.where((at >= BLOCK) | (at <= row), w, 0.0)
        v = jnp.concatenate([vals[i] for i in idx], axis=0)
        return jnp.dot(w.astype(bf16), v, preferred_element_type=f32)

    def group(b, g, q, masked):
        total = None
        for j in range(0, GROUP, pair):
            idx = [table[b, g * GROUP + j + k] for k in range(pair)]
            got = part(q, idx, masked and j == 0)
            total = got if total is None else total + got
        return total

    def one_block(b, _):
        q = q_ref[b]
        acc[...] = group(b, 0, q, True)

        def more(g, _):
            acc[...] += group(b, g, q, False)
            return 0

        lax.fori_loop(1, count[b], more, 0)
        att = (acc[:, :lat_w] / acc[:, lat_w:]).astype(bf16)
        side = jnp.concatenate([att[h * BLOCK : (h + 1) * BLOCK] for h in range(heads)], axis=1)
        out[b] = jnp.dot(side, vup[...], preferred_element_type=f32).astype(bf16)
        return 0

    lax.fori_loop(0, blocks, one_block, 0)


def output_kernel(meta, *refs):
    pieces, (heads, gain, out) = refs[:-3], refs[-3:]
    n = len(pieces)
    order = piece_order(meta, n)
    lhs = jnp.concatenate([heads[p] for p in order], axis=1)
    rhs = jnp.concatenate([p[...] for p in pieces], axis=0)
    acc = jnp.dot(lhs, rhs, preferred_element_type=f32)
    mean_sq = jnp.mean(acc * acc, axis=-1, keepdims=True)
    res = (acc * lax.rsqrt(mean_sq + epsilon) * gain[...]).astype(bf16)
    w = out.shape[2]
    for p in range(n):
        out[p] = res[:, p * w : (p + 1) * w]


def shards(
    tokens,
    query_weight,
    latent_weight,
    query_gain,
    key_gain,
    value_up,
    out_weight,
    out_gain,
    chosen,
):
    rows = tokens.shape[0]
    cols = query_weight.shape[1]
    lat_w = latent_weight.shape[1]
    heads = cols // lat_w
    blocks = rows // BLOCK
    owners = lax.axis_size(KV)
    tp = lax.axis_size(TP)
    sl = BLOCK // tp
    mine = lax.axis_index(KV)
    meta = jnp.stack([lax.axis_index("x"), lax.axis_index("core")]).astype(jnp.int32)

    token_parts = gathered(tokens)

    valid = chosen >= 0
    owner = jnp.maximum(chosen, 0) // blocks
    local = jnp.maximum(chosen, 0) % blocks
    ids = jnp.arange(owners, dtype=jnp.int32)
    hit = (owner[:, :, None] == ids) & valid[:, :, None]
    low = jnp.min(jnp.where(hit, local[:, :, None], blocks), axis=(0, 1))
    high = jnp.max(jnp.where(hit, local[:, :, None], 0), axis=(0, 1))
    wanted = jnp.stack([jnp.minimum(low, blocks - 1), high], axis=1)
    asked = lax.all_to_all(wanted, KV, split_axis=0, concat_axis=0, tiled=True)
    lowest = jnp.sum(jnp.where(hit, low, 0), axis=2)
    far = blocks + owner * PER_OWNER + (local != lowest)
    nothing = blocks + owners * PER_OWNER
    table = jnp.where(valid, jnp.where(owner == mine, local, far), nothing).astype(jnp.int32)
    count = (jnp.sum(valid.astype(jnp.int32), axis=1) + GROUP - 1) // GROUP

    q, latent, send = pl.pallas_call(
        project_kernel,
        out_shape=(
            jax.ShapeDtypeStruct((blocks, heads * BLOCK, lat_w), bf16),
            jax.ShapeDtypeStruct((rows // sl, sl, lat_w), bf16),
            jax.ShapeDtypeStruct((owners, PER_OWNER, sl, lat_w), bf16),
        ),
        in_specs=[SMEM, SMEM] + [VMEM] * (tp + 3),
        out_specs=(VMEM, VMEM, VMEM),
        scratch_shapes=[pltpu.VMEM((tokens.shape[1] * tp, cols + lat_w), bf16)],
        name="project",
    )(meta, asked, *token_parts, query_weight, latent_weight, query_gain[None, :])

    weight_parts = gathered(out_weight)
    got = lax.all_to_all(send, KV, split_axis=0, concat_axis=0, tiled=True)
    got = got.reshape(owners * PER_OWNER, sl, lat_w)
    far_parts = gathered(got)

    vdim = value_up.shape[2]
    mixed_up = jnp.zeros((heads * lat_w, heads * vdim), bf16)
    for h in range(heads):
        mixed_up = mixed_up.at[h * lat_w : (h + 1) * lat_w, h * vdim : (h + 1) * vdim].set(value_up[h])
    scaled_gain = (key_gain * (lat_w**-0.5 * math.log2(math.e)))[None, :]
    slots = blocks + owners * PER_OWNER + 1
    heads_out = pl.pallas_call(
        attend_kernel,
        out_shape=jax.ShapeDtypeStruct((blocks, BLOCK, heads * vdim), bf16),
        in_specs=[SMEM, SMEM] + [VMEM] * (tp + 4),
        out_specs=VMEM,
        scratch_shapes=[
            pltpu.VMEM((slots, BLOCK, lat_w), bf16),
            pltpu.VMEM((slots, BLOCK, 2 * lat_w), bf16),
            pltpu.VMEM((heads * BLOCK, 2 * lat_w), f32),
        ],
        name="attend",
    )(table, count, *far_parts, q, latent.reshape(blocks, BLOCK, lat_w), scaled_gain, mixed_up)

    by_block = lax.all_to_all(heads_out, TP, split_axis=0, concat_axis=0, tiled=True)
    width = out_weight.shape[1] // tp
    res = pl.pallas_call(
        output_kernel,
        out_shape=jax.ShapeDtypeStruct((tp, BLOCK, width), bf16),
        in_specs=[SMEM] + [VMEM] * (tp + 2),
        out_specs=VMEM,
        name="output",
    )(meta, *weight_parts, by_block, out_gain[None, :])
    res = lax.all_to_all(res, TP, split_axis=0, concat_axis=0, tiled=True)
    return res.reshape(rows, width)


def solution(mesh):
    torus = Mesh(mesh.devices.reshape(8, 4, 4, 2), ("kv_0", "kv_1", "x", "core"))
    in_specs = (
        P(KV, TP),
        P(None, TP),
        P(),
        P(),
        P(),
        P(TP, None, None),
        P(TP, None),
        P(),
        P(KV, None),
    )
    return jax.shard_map(
        shards, mesh=torus, in_specs=in_specs, out_specs=P(KV, TP), check_vma=False
    )
```

```python
import math

import jax
import jax.numpy as jnp
from jax import lax
from jax.experimental import pallas as pl
from jax.experimental.pallas import tpu as pltpu
from jax.sharding import Mesh
from jax.sharding import PartitionSpec as P

BLOCK = 128
PER_OWNER = 2
KV = ("kv_0", "kv_1")
TP = ("x", "core")
GROUP = 4
ROWS = 512


epsilon = 1e-06
f32 = jnp.float32
bf16 = jnp.bfloat16

VMEM = pl.BlockSpec(memory_space=pltpu.VMEM)
SMEM = pl.BlockSpec(memory_space=pltpu.SMEM)


def shifted(part, axis, step):
    n = lax.axis_size(axis)
    return lax.ppermute(part, axis, [(i, (i + step) % n) for i in range(n)])


def gathered(part):
    steps = range(1, lax.axis_size("x"))
    along_x = [part] + [shifted(part, "x", d) for d in steps]
    return along_x + [shifted(p, "core", 1) for p in along_x]


def exchanged(parts, axes):
    return lax.all_to_all(parts, axes, split_axis=0, concat_axis=0, tiled=True)


def normed(values, gain_row):
    wide = values.astype(f32)
    mean_sq = jnp.mean(wide * wide, axis=-1, keepdims=True)
    return (wide * lax.rsqrt(mean_sq + epsilon) * gain_row).astype(bf16)


def side_by_side(ref, *at):
    return jnp.concatenate([ref[(i, *at)] for i in range(ref.shape[0])], axis=1)


def latent_kernel(asked, tok, lw, lat_out, send_out):
    lat = jnp.dot(side_by_side(tok, 1), lw[...], preferred_element_type=f32).astype(bf16)
    lat_out[...] = lat.reshape(lat_out.shape)

    def serve(o, _):
        for s in range(PER_OWNER):
            send_out[o, s] = lat_out[asked[o, s]]
        return 0

    lax.fori_loop(0, send_out.shape[0], serve, 0, unroll=8)


def pick_kernel(table, own, got, out):
    blocks = own.shape[0]
    picks = out.shape[1]

    def pick(i, _):
        t, c = i // picks, i % picks
        at = table[t, c]
        far = got[jnp.maximum(at - blocks, 0)]
        near = own[jnp.minimum(at, blocks - 1)]
        out[t, c] = jnp.where(at < blocks, near, far)
        return 0

    lax.fori_loop(0, out.shape[0] * picks, pick, 0, unroll=8)


def query_kernel(tok, *refs):
    pieces, (gain, out) = refs[:-2], refs[-2:]
    lhs = side_by_side(tok, 0)
    width = gain.shape[1]
    at = 0
    for piece in pieces:
        acc = jnp.dot(lhs, piece[...], preferred_element_type=f32).astype(bf16)
        for h in range(acc.shape[1] // width):
            out[at] = normed(acc[:, h * width : (h + 1) * width], gain[...])
            at += 1


def attend_kernel(count, q_ref, kv, kgain, out, acc):
    n = kv.shape[0]
    sl, width = kv.shape[2], kv.shape[3]
    heads = q_ref.shape[0]
    per = ROWS // BLOCK
    gain = kgain[...] * (width**-0.5 * math.log2(math.e))
    valid_count = count[0]

    def group(g, first):
        keys, vals = [], []
        for j in range(GROUP):
            c = g * GROUP + j
            lat = jnp.concatenate([kv[s, c] for s in range(n)], axis=0)
            on = c < valid_count
            lat = jnp.where(on, lat, jnp.zeros_like(lat))
            ones = jnp.where(on, jnp.ones_like(lat), jnp.zeros_like(lat))
            keys.append(normed(lat, gain))
            vals.append(jnp.concatenate([lat, ones], axis=1))
        k = jnp.concatenate(keys, axis=0)
        v = jnp.concatenate(vals, axis=0)
        for r in range(heads // per):
            q = jnp.concatenate([q_ref[r * per + h] for h in range(per)], axis=0)
            s = lax.dot_general(q, k, (((1,), (1,)), ((), ())), preferred_element_type=f32)
            w = jnp.exp2(s)
            if first:
                at = lax.broadcasted_iota(jnp.int32, (ROWS, BLOCK), 1)
                row = lax.broadcasted_iota(jnp.int32, (ROWS, BLOCK), 0) & (BLOCK - 1)
                own = jnp.where(at <= row, w[:, :BLOCK], 0.0)
                w = jnp.concatenate([own, w[:, BLOCK:]], axis=1)
            got = jnp.dot(w.astype(bf16), v, preferred_element_type=f32)
            if first:
                acc[r] = got
            else:
                acc[r] += got

    group(0, True)

    def more(g, _):
        group(g, False)
        return 0

    lax.fori_loop(1, (valid_count + GROUP - 1) // GROUP, more, 0)
    for r in range(heads // per):
        res = (acc[r, :, :width] / acc[r, :, width:]).astype(bf16)
        out[r * per : (r + 1) * per] = res.reshape(per, BLOCK, width)


def output_kernel(*refs):
    pieces, (att, gain, out) = refs[:-3], refs[-3:]
    model = gain.shape[1]
    width = att.shape[2]
    sides = []
    for i, piece in enumerate(pieces):
        up = piece[:, model:]
        low = jnp.dot(att[2 * i], up, preferred_element_type=f32)
        high = jnp.dot(att[2 * i + 1], up, preferred_element_type=f32)
        lane = lax.broadcasted_iota(jnp.int32, low.shape, 1)
        sides.append(jnp.where(lane < up.shape[1] // 2, low, high).astype(bf16))
    lhs = jnp.concatenate(sides, axis=1)
    rhs = jnp.concatenate([p[:, :model] for p in pieces], axis=0)
    acc = jnp.dot(lhs, rhs, preferred_element_type=f32)
    mean_sq = jnp.mean(acc * acc, axis=-1, keepdims=True)
    res = (acc * lax.rsqrt(mean_sq + epsilon) * gain[...]).astype(bf16)
    w = out.shape[2]
    for p in range(out.shape[0]):
        out[p] = res[:, p * w : (p + 1) * w]


def shards(
    tokens,
    query_weight,
    latent_weight,
    query_gain,
    key_gain,
    value_up,
    out_weight,
    out_gain,
    chosen,
):
    rows, feats = tokens.shape
    lat_w = latent_weight.shape[1]
    blocks = rows // BLOCK
    picks = chosen.shape[1]
    owners = lax.axis_size(KV)
    tp = lax.axis_size(TP)
    sl = BLOCK // tp
    mine = lax.axis_index(KV)
    heads = query_weight.shape[1] // lat_w * tp

    with jax.named_scope("wanted"):
        valid = chosen >= 0
        owner = jnp.maximum(chosen, 0) // blocks
        local = jnp.maximum(chosen, 0) % blocks
        ids = jnp.arange(owners, dtype=jnp.int32)
        hit = (owner[:, :, None] == ids) & valid[:, :, None]
        low = jnp.min(jnp.where(hit, local[:, :, None], blocks), axis=(0, 1))
        high = jnp.max(jnp.where(hit, local[:, :, None], 0), axis=(0, 1))
        wanted = jnp.stack([jnp.minimum(low, blocks - 1), high], axis=1)
        asked = exchanged(wanted, KV)
        lowest = jnp.sum(jnp.where(hit, low, 0), axis=2)
        far = blocks + owner * PER_OWNER + (local != lowest)
        table = jnp.where(valid, jnp.where(owner == mine, local, far), 0).astype(jnp.int32)
        my_block = lax.axis_index(TP)
        count = lax.dynamic_slice_in_dim(jnp.sum(valid.astype(jnp.int32), axis=1), my_block, 1)

    with jax.named_scope("tokens"):
        by_block = tokens.reshape(blocks, BLOCK, feats)
        by_slice = tokens.reshape(blocks, tp, sl, feats).swapaxes(0, 1).reshape(tp, BLOCK, feats)
        tok = exchanged(jnp.stack([by_block, by_slice], axis=1), TP)

    with jax.named_scope("queries"):
        query_parts = gathered(query_weight)

    latent, send = pl.pallas_call(
        latent_kernel,
        out_shape=(
            jax.ShapeDtypeStruct((blocks, sl, lat_w), bf16),
            jax.ShapeDtypeStruct((owners, PER_OWNER, sl, lat_w), bf16),
        ),
        in_specs=[SMEM, VMEM, VMEM],
        out_specs=(VMEM, VMEM),
        name="latent",
    )(asked, tok, latent_weight)

    with jax.named_scope("blocks"):
        got = exchanged(send, KV).reshape(owners * PER_OWNER, sl, lat_w)

    picked = pl.pallas_call(
        pick_kernel,
        out_shape=jax.ShapeDtypeStruct((tp, picks, sl, lat_w), bf16),
        in_specs=[SMEM, VMEM, VMEM],
        out_specs=VMEM,
        name="pick",
    )(table, latent, got)

    with jax.named_scope("picked"):
        kv = exchanged(picked, TP)

    with jax.named_scope("weights"):
        up = value_up.swapaxes(0, 1).reshape(lat_w, -1)
        weight_parts = gathered(jnp.concatenate([out_weight, up], axis=1))

    q = pl.pallas_call(
        query_kernel,
        out_shape=jax.ShapeDtypeStruct((heads, BLOCK, lat_w), bf16),
        in_specs=[VMEM] * (tp + 2),
        out_specs=VMEM,
        name="query",
    )(tok, *query_parts, query_gain[None, :])

    attended = pl.pallas_call(
        attend_kernel,
        out_shape=jax.ShapeDtypeStruct((heads, BLOCK, lat_w), bf16),
        in_specs=[SMEM] + [VMEM] * 3,
        out_specs=VMEM,
        scratch_shapes=[pltpu.VMEM((heads * BLOCK // ROWS, ROWS, 2 * lat_w), f32)],
        name="attend",
    )(count, q, kv, key_gain[None, :])

    width = out_weight.shape[1] // tp
    res = pl.pallas_call(
        output_kernel,
        out_shape=jax.ShapeDtypeStruct((tp, BLOCK, width), bf16),
        in_specs=[VMEM] * (tp + 2),
        out_specs=VMEM,
        name="output",
    )(*weight_parts, attended, out_gain[None, :])
    with jax.named_scope("result"):
        return exchanged(res, TP).reshape(rows, width)


def solution(mesh):
    torus = Mesh(mesh.devices.reshape(8, 4, 4, 2), ("kv_0", "kv_1", "x", "core"))
    in_specs = (
        P(KV, TP),
        P(None, TP),
        P(),
        P(),
        P(),
        P(TP, None, None),
        P(TP, None),
        P(),
        P(KV, None),
    )
    return jax.shard_map(
        shards, mesh=torus, in_specs=in_specs, out_specs=P(KV, TP), check_vma=False
    )
```

```python
import math

import jax
import jax.numpy as jnp
from jax import lax
from jax.experimental import pallas as pl
from jax.experimental.pallas import tpu as pltpu
from jax.sharding import Mesh
from jax.sharding import PartitionSpec as P


BLOCK = 128
PER_OWNER = 2
KV = ("kv_0", "kv_1")
TP = ("x", "core")
CHIPS = 4
CORES = 2
ROWS = 512

SHIFTS = [(0, 0), (0, 1), (1, 0), (1, 1), (3, 0), (3, 1), (2, 0), (2, 1)]


epsilon = 1e-06
f32 = jnp.float32
bf16 = jnp.bfloat16
i32 = jnp.int32

VMEM = pl.BlockSpec(memory_space=pltpu.VMEM)
SMEM = pl.BlockSpec(memory_space=pltpu.SMEM)


def place(shift, sign):
    dx, dc = shift
    x, core = lax.axis_index("x"), lax.axis_index("core")
    other = core if dc == 0 else 1 - core
    return CORES * lax.rem(x + sign * dx + CHIPS, CHIPS) + other


def moved(part, shift):
    dx, dc = shift
    if shift == (0, 0):
        return part
    pairs = [
        (CORES * x + c, CORES * ((x + dx) % CHIPS) + (c ^ dc))
        for x in range(CHIPS)
        for c in range(CORES)
    ]
    return lax.ppermute(part, TP, pairs)


def gathered(part):
    along_x = {0: part}
    for dx in (1, 3, 2):
        along_x[dx] = moved(part, (dx, 0))
    return [moved(along_x[dx], (0, dc)) for dx, dc in SHIFTS]


def normed(values, gain_row):
    wide = values.astype(f32)
    mean_sq = jnp.mean(wide * wide, axis=-1, keepdims=True)
    return (wide * lax.rsqrt(mean_sq + epsilon) * gain_row).astype(bf16)


def side_by_side(ref):
    return jnp.concatenate([ref[i] for i in range(ref.shape[0])], axis=1)


def prepare_kernel(tokens, chosen, *outs):
    bufs, (wanted, table, count) = outs[:-3], outs[-3:]
    tp = len(bufs)
    blocks = tokens.shape[0] // BLOCK
    sl = BLOCK // tp
    owners = wanted.shape[0]
    for buf, shift in zip(bufs, SHIFTS):
        dest = place(shift, 1)
        buf[0] = tokens[pl.ds(pl.multiple_of(dest * BLOCK, BLOCK), BLOCK), :]
        for b in range(blocks):
            at = pl.multiple_of(b * BLOCK + dest * sl, sl)
            buf[1, b * sl : (b + 1) * sl, :] = tokens[pl.ds(at, sl), :]
    mine = lax.axis_index(KV[0]) * lax.axis_size(KV[1]) + lax.axis_index(KV[1])
    c = chosen[...]
    valid = c >= 0
    owner = lax.shift_right_arithmetic(c, blocks.bit_length() - 1)
    local = c & (blocks - 1)
    lowest = jnp.zeros_like(c)
    lane = lax.broadcasted_iota(i32, (1, wanted.shape[2]), 1)
    for o in range(owners):
        hit = owner == o
        low = jnp.min(jnp.where(hit, local, blocks - 1), keepdims=True)
        high = jnp.max(jnp.where(hit, local, 0), keepdims=True)
        wanted[o] = jnp.where(lane == 0, low, high)
        lowest = jnp.where(hit, low, lowest)
    far = blocks + owner * PER_OWNER + jnp.where(local == lowest, 0, 1)
    table[...] = jnp.where(valid, jnp.where(owner == mine, local, far), 0)
    count[...] = jnp.broadcast_to(
        jnp.sum(jnp.where(valid, 1.0, 0.0), axis=1, keepdims=True).astype(i32), count.shape
    )


def latent_kernel(asked, lw, *refs):
    toks, (lat_out, send_out, tok) = refs[:-3], refs[-3:]
    for part, shift in zip(toks, SHIFTS):
        tok[place(shift, -1)] = part[1]
    lat = jnp.dot(side_by_side(tok), lw[...], preferred_element_type=f32).astype(bf16)
    lat_out[...] = lat.reshape(lat_out.shape)
    for o in range(send_out.shape[0]):
        for s in range(PER_OWNER):
            send_out[o, s] = lat_out[asked[o, 0, s]]


def pick_kernel(table, own, got, *refs):
    outs, pool = refs[:-1], refs[-1]
    blocks = own.shape[0]
    pool[:blocks] = own[...]
    pool[blocks:] = got[...]
    for out, shift in zip(outs, SHIFTS):
        dest = place(shift, 1)
        for c in range(out.shape[0]):
            out[c] = pool[table[dest, c]]


def query_kernel(gain, *refs):
    out, tok = refs[-2:]
    n = len(SHIFTS)
    toks, pieces = refs[:n], refs[n:-2]
    for part, shift in zip(toks, SHIFTS):
        tok[place(shift, -1)] = part[0]
    lhs = side_by_side(tok)
    width = gain.shape[1]
    at = 0
    for piece in pieces:
        acc = jnp.dot(lhs, piece[...], preferred_element_type=f32).astype(bf16)
        for h in range(acc.shape[1] // width):
            out[at] = normed(acc[:, h * width : (h + 1) * width], gain[...])
            at += 1


def add_piece(q_ref, kv, kgain, count, src, acc_in, acc):
    picks, sl, width = kv.shape
    keys = picks * sl
    per = ROWS // BLOCK
    lat = kv[...].reshape(keys, width)
    on = lax.broadcasted_iota(i32, (keys, width), 0) < count * sl
    lat = jnp.where(on, lat, jnp.zeros_like(lat))
    ones = jnp.where(on, jnp.ones_like(lat), jnp.zeros_like(lat))
    k = normed(lat, kgain[...] * (width**-0.5 * math.log2(math.e)))
    v = jnp.concatenate([lat, ones], axis=1)
    at = lax.broadcasted_iota(i32, (ROWS, BLOCK), 1)
    row = lax.broadcasted_iota(i32, (ROWS, BLOCK), 0) & (BLOCK - 1)
    for r in range(q_ref.shape[0] // per):
        q = jnp.concatenate([q_ref[r * per + h] for h in range(per)], axis=0)
        s = lax.dot_general(q, k, (((1,), (1,)), ((), ())), preferred_element_type=f32)
        w = jnp.exp2(s)
        own = jnp.where((at >= sl) | (at + src * sl <= row), w[:, :BLOCK], 0.0)
        w = jnp.concatenate([own, w[:, BLOCK:]], axis=1).astype(bf16)
        got = jnp.dot(w, v, preferred_element_type=f32)
        acc[r] = got if acc_in is None else acc_in[r] + got


def attend_kernel(shifts, first, last, count, q_ref, kgain, *refs):
    n = len(shifts)
    pieces, rest = refs[:n], refs[n:]
    acc_in, rest = (None, rest) if first else (rest[0], rest[1:])
    acc = rest[-1]
    here = count[place((0, 0), 1), 0]
    for piece, shift in zip(pieces, shifts):
        add_piece(q_ref, piece, kgain, here, place(shift, -1), acc_in, acc)
        acc_in = acc
    if last:
        out = rest[0]
        width = out.shape[2]
        per = ROWS // BLOCK
        for r in range(out.shape[0] // per):
            res = (acc[r, :, :width] / acc[r, :, width:]).astype(bf16)
            out[r * per : (r + 1) * per] = res.reshape(per, BLOCK, width)


def output_kernel(*refs):
    pieces, (att, gain, out) = refs[:-3], refs[-3:]
    model = gain.shape[1]
    sides = []
    for i, piece in enumerate(pieces):
        up = piece[:, model:]
        low = jnp.dot(att[2 * i], up, preferred_element_type=f32)
        high = jnp.dot(att[2 * i + 1], up, preferred_element_type=f32)
        lane = lax.broadcasted_iota(i32, low.shape, 1)
        sides.append(jnp.where(lane < up.shape[1] // 2, low, high).astype(bf16))
    lhs = jnp.concatenate(sides, axis=1)
    rhs = jnp.concatenate([p[:, :model] for p in pieces], axis=0)
    acc = jnp.dot(lhs, rhs, preferred_element_type=f32)
    mean_sq = jnp.mean(acc * acc, axis=-1, keepdims=True)
    res = (acc * lax.rsqrt(mean_sq + epsilon) * gain[...]).astype(bf16)
    w = out.shape[2]
    for p in range(out.shape[0]):
        out[p] = res[:, p * w : (p + 1) * w]


def shape(dims, kind=bf16):
    return jax.ShapeDtypeStruct(dims, kind)


def shards(
    tokens,
    query_weight,
    latent_weight,
    query_gain,
    key_gain,
    value_up,
    out_weight,
    out_gain,
    chosen,
):
    rows, feats = tokens.shape
    lat_w = latent_weight.shape[1]
    blocks = rows // BLOCK
    picks = chosen.shape[1]
    owners = lax.axis_size(KV)
    tp = len(SHIFTS)
    sl = BLOCK // tp
    heads = query_weight.shape[1] // lat_w * tp

    *bufs, wanted, table, count = pl.pallas_call(
        prepare_kernel,
        out_shape=[shape((2, BLOCK, feats))] * tp
        + [shape((owners, 1, BLOCK), i32), shape((blocks, picks), i32), shape((blocks, BLOCK), i32)],
        in_specs=[VMEM, VMEM],
        out_specs=[VMEM] * (tp + 3),
        name="prepare",
    )(tokens, chosen)

    toks = [moved(b, s) for b, s in zip(bufs, SHIFTS)]
    asked = lax.all_to_all(wanted, KV, split_axis=0, concat_axis=0, tiled=True)

    query_parts = gathered(query_weight)

    latent, send = pl.pallas_call(
        latent_kernel,
        out_shape=(shape((blocks, sl, lat_w)), shape((owners, PER_OWNER, sl, lat_w))),
        in_specs=[SMEM] + [VMEM] * (tp + 1),
        out_specs=(VMEM, VMEM),
        scratch_shapes=[pltpu.VMEM((tp, BLOCK, feats), bf16)],
        name="latent",
    )(asked, latent_weight, *toks)

    got = lax.all_to_all(send, KV, split_axis=0, concat_axis=0, tiled=True)
    got = got.reshape(owners * PER_OWNER, sl, lat_w)

    picked = pl.pallas_call(
        pick_kernel,
        out_shape=[shape((picks, sl, lat_w))] * tp,
        in_specs=[SMEM, VMEM, VMEM],
        out_specs=[VMEM] * tp,
        scratch_shapes=[pltpu.VMEM((blocks + owners * PER_OWNER, sl, lat_w), bf16)],
        name="pick",
    )(table, latent, got)
    kv = {}
    for part, s in zip(picked, SHIFTS):
        kv[s] = moved(part, s)

    up = value_up.swapaxes(0, 1).reshape(lat_w, -1)
    weight_parts = gathered(jnp.concatenate([out_weight, up], axis=1))

    q = pl.pallas_call(
        query_kernel,
        out_shape=shape((heads, BLOCK, lat_w)),
        in_specs=[VMEM] * (2 * tp + 1),
        out_specs=VMEM,
        scratch_shapes=[pltpu.VMEM((tp, BLOCK, feats), bf16)],
        name="query",
    )(query_gain[None, :], *toks, *query_parts)

    sums = (heads * BLOCK // ROWS, ROWS, 2 * lat_w)
    state = []
    for shifts in (SHIFTS[:2], SHIFTS[2:6], SHIFTS[6:]):
        first, last = shifts[0] == SHIFTS[0], shifts[-1] == SHIFTS[-1]

        def kernel(*refs, shifts=shifts, first=first, last=last):
            attend_kernel(shifts, first, last, *refs)

        state = [
            pl.pallas_call(
                kernel,
                out_shape=shape((heads, BLOCK, lat_w)) if last else shape(sums, f32),
                in_specs=[SMEM] + [VMEM] * (2 + len(shifts) + len(state)),
                out_specs=VMEM,
                scratch_shapes=[pltpu.VMEM(sums, f32)] if last else [],
            )(count, q, key_gain[None, :], *[kv[s] for s in shifts], *state)
        ]

    width = out_weight.shape[1] // tp
    res = pl.pallas_call(
        output_kernel,
        out_shape=shape((tp, BLOCK, width)),
        in_specs=[VMEM] * (tp + 2),
        out_specs=VMEM,
        name="output",
    )(*weight_parts, state[0], out_gain[None, :])
    res = lax.all_to_all(res, TP, split_axis=0, concat_axis=0, tiled=True)
    return res.reshape(rows, width)


def solution(mesh):
    torus = Mesh(mesh.devices.reshape(8, CHIPS, 4, CORES), ("kv_0", "kv_1", "x", "core"))
    in_specs = (
        P(KV, TP),
        P(None, TP),
        P(),
        P(),
        P(),
        P(TP, None, None),
        P(TP, None),
        P(),
        P(KV, None),
    )
    return jax.shard_map(
        shards, mesh=torus, in_specs=in_specs, out_specs=P(KV, TP), check_vma=False
    )
```

```python
import math

import jax
import jax.numpy as jnp
from jax import lax
from jax.experimental import pallas as pl
from jax.experimental.pallas import tpu as pltpu
from jax.sharding import Mesh
from jax.sharding import PartitionSpec as P


BLOCK = 128
PER_OWNER = 2
KV = ("kv_0", "kv_1")
TP = ("x", "core")
CHIPS = 4
CORES = 2
ROWS = 512
LANES = 256

STEPS = (0, 1, 3, 2)
SOURCES = [(dx, dc) for dc in (0, 1) for dx in STEPS]


epsilon = 1e-06
f32 = jnp.float32
bf16 = jnp.bfloat16
i32 = jnp.int32

VMEM = pl.BlockSpec(memory_space=pltpu.VMEM)
SMEM = pl.BlockSpec(memory_space=pltpu.SMEM)
ANY = pl.BlockSpec(memory_space=pl.ANY)


def chip_at(step):
    return lax.rem(lax.axis_index("x") + step + CHIPS, CHIPS)


def came_from(source):
    dx, dc = source
    core = lax.axis_index("core")
    return CORES * chip_at(-dx) + (core if dc == 0 else 1 - core)


def over_x(parts):
    out = [parts[0]]
    for part, dx in zip(parts[1:], STEPS[1:]):
        out.append(lax.ppermute(part, "x", [(i, (i + dx) % CHIPS) for i in range(CHIPS)]))
    return out


def with_partner(parts):
    return parts + [lax.ppermute(p, "core", [(0, 1), (1, 0)]) for p in parts]


def normed(values, gain_row):
    wide = values.astype(f32)
    mean_sq = jnp.mean(wide * wide, axis=-1, keepdims=True)
    return (wide * lax.rsqrt(mean_sq + epsilon) * gain_row).astype(bf16)


def side_by_side(ref):
    return jnp.concatenate([ref[i] for i in range(ref.shape[0])], axis=1)


def prepare_kernel(tokens, chosen, qw, ow, up, *outs):
    bufs, (bundle, wanted, table, count) = outs[:-4], outs[-4:]
    blocks = tokens.shape[0] // BLOCK
    sl = BLOCK // (CHIPS * CORES)
    owners = wanted.shape[0]
    for buf, dx in zip(bufs, STEPS):
        for core in range(CORES):
            dest = CORES * chip_at(dx) + core
            buf[core, 0] = tokens[pl.ds(pl.multiple_of(dest * BLOCK, BLOCK), BLOCK), :]
            for b in range(blocks):
                at = pl.multiple_of(b * BLOCK + dest * sl, sl)
                buf[core, 1, b * sl : (b + 1) * sl, :] = tokens[pl.ds(at, sl), :]
    at = qw.shape[0]
    bundle[:at] = qw[...]
    for c in range(0, ow.shape[1], LANES):
        bundle[at : at + ow.shape[0]] = ow[:, c : c + LANES]
        at += ow.shape[0]
    bundle[at:, : up.shape[2]] = up[0]
    bundle[at:, up.shape[2] :] = up[1]
    mine = lax.axis_index(KV[0]) * lax.axis_size(KV[1]) + lax.axis_index(KV[1])
    c = chosen[...]
    valid = c >= 0
    owner = lax.shift_right_arithmetic(c, blocks.bit_length() - 1)
    local = c & (blocks - 1)
    lowest = jnp.zeros_like(c)
    lane = lax.broadcasted_iota(i32, (1, wanted.shape[2]), 1)
    for o in range(owners):
        hit = owner == o
        low = jnp.min(jnp.where(hit, local, blocks - 1), keepdims=True)
        high = jnp.max(jnp.where(hit, local, 0), keepdims=True)
        wanted[o] = jnp.where(lane == 0, low, high)
        lowest = jnp.where(hit, low, lowest)
    far = blocks + owner * PER_OWNER + jnp.where(local == lowest, 0, 1)
    table[...] = jnp.where(valid, jnp.where(owner == mine, local, far), 0)
    count[...] = jnp.broadcast_to(
        jnp.sum(jnp.where(valid, 1.0, 0.0), axis=1, keepdims=True).astype(i32), count.shape
    )


def latent_kernel(asked, lw, *refs):
    toks, (lat_out, send_out, tok) = refs[:-3], refs[-3:]
    for part, source in zip(toks, SOURCES):
        tok[came_from(source)] = part[lax.axis_index("core"), 1]
    lat = jnp.dot(side_by_side(tok), lw[...], preferred_element_type=f32).astype(bf16)
    lat_out[...] = lat.reshape(lat_out.shape)
    for o in range(send_out.shape[0]):
        for s in range(PER_OWNER):
            send_out[o, s] = lat_out[asked[o, 0, s]]


def pick_kernel(table, own, got, *refs):
    outs, pool = refs[:-1], refs[-1]
    blocks = own.shape[0]
    pool[:blocks] = own[...]
    pool[blocks:] = got[...]
    for out, dx in zip(outs, STEPS):
        for core in range(CORES):
            dest = CORES * chip_at(dx) + core
            for c in range(out.shape[1]):
                out[core, c] = pool[table[dest, c]]


def query_kernel(gain, *refs):
    n = len(SOURCES)
    toks, pieces, (out, tok, weights, sem) = refs[:n], refs[n : 2 * n], refs[2 * n :]
    fetch = [
        pltpu.make_async_copy(p.at[pl.ds(0, weights.shape[1])], weights.at[i], sem.at[i])
        for i, p in enumerate(pieces)
    ]
    for copy in fetch:
        copy.start()
    for part, source in zip(toks, SOURCES):
        tok[came_from(source)] = part[lax.axis_index("core"), 0]
    lhs = side_by_side(tok)
    width = gain.shape[1]
    heads = out.shape[0] // n
    for i in range(n):
        fetch[i].wait()
        acc = jnp.dot(lhs, weights[i], preferred_element_type=f32).astype(bf16)
        for h in range(heads):
            out[i * heads + h] = normed(acc[:, h * width : (h + 1) * width], gain[...])


def attend_kernel(count, q_ref, kgain, ogain, *refs):
    n = len(SOURCES)
    pieces, bundles, (out, kv, weights, acc, kv_sem, weight_sem) = refs[:n], refs[n : 2 * n], refs[2 * n :]
    mine = lax.axis_index("core")
    fetch = [pltpu.make_async_copy(p.at[mine], kv.at[i], kv_sem.at[i]) for i, p in enumerate(pieces)]
    first = bundles[0].shape[0] - weights.shape[1]
    later = [
        pltpu.make_async_copy(b.at[pl.ds(first, weights.shape[1])], weights.at[i], weight_sem.at[i])
        for i, b in enumerate(bundles)
    ]
    for copy in fetch + later:
        copy.start()
    _, picks, sl, width = kv.shape
    keys = picks * sl
    heads = q_ref.shape[0]
    per = ROWS // BLOCK
    here = count[came_from((0, 0)), 0]
    gain = kgain[...] * (width**-0.5 * math.log2(math.e))
    on = lax.broadcasted_iota(i32, (keys, width), 0) < here * sl
    at = lax.broadcasted_iota(i32, (ROWS, BLOCK), 1)
    row = lax.broadcasted_iota(i32, (ROWS, BLOCK), 0) & (BLOCK - 1)
    for i, source in enumerate(SOURCES):
        fetch[i].wait()
        src = came_from(source)
        lat = kv[i].reshape(keys, width)
        lat = jnp.where(on, lat, jnp.zeros_like(lat))
        ones = jnp.where(on, jnp.ones_like(lat), jnp.zeros_like(lat))
        k = normed(lat, gain)
        v = jnp.concatenate([lat, ones], axis=1)
        for r in range(heads // per):
            q = jnp.concatenate([q_ref[r * per + h] for h in range(per)], axis=0)
            s = lax.dot_general(q, k, (((1,), (1,)), ((), ())), preferred_element_type=f32)
            w = jnp.exp2(s)
            own = jnp.where((at >= sl) | (at + src * sl <= row), w[:, :BLOCK], 0.0)
            w = jnp.concatenate([own, w[:, BLOCK:]], axis=1).astype(bf16)
            got = jnp.dot(w, v, preferred_element_type=f32)
            acc[r] = got if i == 0 else acc[r] + got
    for copy in later:
        copy.wait()
    model = ogain.shape[1]
    total = None
    for i in range(n):
        block = weights[i]
        rows = model // LANES * BLOCK
        up = jnp.concatenate([block[rows:, :width], block[rows:, width:]], axis=0)
        halves = []
        for h in (CORES * i, CORES * i + 1):
            r, k = h // per, h % per
            sums = acc[r, k * BLOCK : (k + 1) * BLOCK, :]
            att = (sums[:, :width] / sums[:, width:]).astype(bf16)
            halves.append(
                lax.dot_general(att, up, (((1,), (1,)), ((), ())), preferred_element_type=f32)
            )
        lane = lax.broadcasted_iota(i32, halves[0].shape, 1)
        side = jnp.where(lane < width // CORES, halves[0], halves[1]).astype(bf16)
        proj = jnp.concatenate(
            [block[c * BLOCK : (c + 1) * BLOCK] for c in range(model // LANES)], axis=1
        )
        part = jnp.dot(side, proj, preferred_element_type=f32)
        total = part if total is None else total + part
    mean_sq = jnp.mean(total * total, axis=-1, keepdims=True)
    res = (total * lax.rsqrt(mean_sq + epsilon) * ogain[...]).astype(bf16)
    w = out.shape[2]
    for p in range(out.shape[0]):
        out[p] = res[:, p * w : (p + 1) * w]


def shape(dims, kind=bf16):
    return jax.ShapeDtypeStruct(dims, kind)


def shards(
    tokens,
    query_weight,
    latent_weight,
    query_gain,
    key_gain,
    value_up,
    out_weight,
    out_gain,
    chosen,
):
    rows, feats = tokens.shape
    lat_w = latent_weight.shape[1]
    blocks = rows // BLOCK
    picks = chosen.shape[1]
    owners = lax.axis_size(KV)
    tp = len(SOURCES)
    sl = BLOCK // tp
    heads = query_weight.shape[1] // lat_w * tp
    q_rows = query_weight.shape[0]
    late_rows = (out_weight.size + value_up.size) // LANES

    *bufs, bundle, wanted, table, count = pl.pallas_call(
        prepare_kernel,
        out_shape=[shape((CORES, 2, BLOCK, feats))] * CHIPS
        + [
            shape((q_rows + late_rows, LANES)),
            shape((owners, 1, BLOCK), i32),
            shape((blocks, picks), i32),
            shape((blocks, BLOCK), i32),
        ],
        in_specs=[VMEM] * 5,
        out_specs=[VMEM] * (CHIPS + 4),
        name="prepare",
    )(tokens, chosen, query_weight, out_weight, value_up.swapaxes(1, 2))

    toks_x = over_x(bufs)
    bundles_x = over_x([bundle] * CHIPS)
    asked = lax.all_to_all(wanted, KV, split_axis=0, concat_axis=0, tiled=True)
    toks = with_partner(toks_x)

    latent, send = pl.pallas_call(
        latent_kernel,
        out_shape=(shape((blocks, sl, lat_w)), shape((owners, PER_OWNER, sl, lat_w))),
        in_specs=[SMEM] + [VMEM] * (tp + 1),
        out_specs=(VMEM, VMEM),
        scratch_shapes=[pltpu.VMEM((tp, BLOCK, feats), bf16)],
        name="latent",
    )(asked, latent_weight, *toks)

    got = lax.all_to_all(send, KV, split_axis=0, concat_axis=0, tiled=True)
    got = got.reshape(owners * PER_OWNER, sl, lat_w)

    picked = pl.pallas_call(
        pick_kernel,
        out_shape=[shape((CORES, picks, sl, lat_w))] * CHIPS,
        in_specs=[SMEM, VMEM, VMEM],
        out_specs=[VMEM] * CHIPS,
        scratch_shapes=[pltpu.VMEM((blocks + owners * PER_OWNER, sl, lat_w), bf16)],
        name="pick",
    )(table, latent, got)
    kv = with_partner(over_x(picked))
    bundles = with_partner(bundles_x)

    q = pl.pallas_call(
        query_kernel,
        out_shape=shape((heads, BLOCK, lat_w)),
        in_specs=[VMEM] * (tp + 1) + [ANY] * tp,
        out_specs=VMEM,
        scratch_shapes=[
            pltpu.VMEM((tp, BLOCK, feats), bf16),
            pltpu.VMEM((tp, q_rows, LANES), bf16),
            pltpu.SemaphoreType.DMA((tp,)),
        ],
        name="query",
    )(query_gain[None, :], *toks, *bundles)

    width = out_weight.shape[1] // tp
    res = pl.pallas_call(
        attend_kernel,
        out_shape=shape((tp, BLOCK, width)),
        in_specs=[SMEM] + [VMEM] * 3 + [ANY] * (2 * tp),
        out_specs=VMEM,
        scratch_shapes=[
            pltpu.VMEM((tp, picks, sl, lat_w), bf16),
            pltpu.VMEM((tp, late_rows, LANES), bf16),
            pltpu.VMEM((heads * BLOCK // ROWS, ROWS, 2 * lat_w), f32),
            pltpu.SemaphoreType.DMA((tp,)),
            pltpu.SemaphoreType.DMA((tp,)),
        ],
        name="attend",
    )(count, q, key_gain[None, :], out_gain[None, :], *kv, *bundles)

    res = lax.all_to_all(res, TP, split_axis=0, concat_axis=0, tiled=True)
    return res.reshape(rows, width)


def solution(mesh):
    torus = Mesh(mesh.devices.reshape(8, 4, CHIPS, CORES), ("kv_0", "kv_1", "x", "core"))
    in_specs = (
        P(KV, TP),
        P(None, TP),
        P(),
        P(),
        P(),
        P(TP, None, None),
        P(TP, None),
        P(),
        P(KV, None),
    )
    return jax.shard_map(
        shards, mesh=torus, in_specs=in_specs, out_specs=P(KV, TP), check_vma=False
    )
```

```python
import math

import jax
import jax.numpy as jnp
from jax import lax
from jax.experimental import pallas as pl
from jax.experimental.pallas import tpu as pltpu
from jax.sharding import Mesh
from jax.sharding import PartitionSpec as P


BLOCK = 128
PER_OWNER = 2
KV = ("kv_0", "kv_1")
TP = ("x", "core")
CHIPS = 4
CORES = 2
ROWS = 512
LANES = 256

STEPS = (0, 1, 3, 2)
SOURCES = [(dx, dc) for dc in (0, 1) for dx in STEPS]


epsilon = 1e-06
f32 = jnp.float32
bf16 = jnp.bfloat16
i32 = jnp.int32

VMEM = pl.BlockSpec(memory_space=pltpu.VMEM)
SMEM = pl.BlockSpec(memory_space=pltpu.SMEM)
ANY = pl.BlockSpec(memory_space=pl.ANY)


def chip_at(step):
    return lax.rem(lax.axis_index("x") + step + CHIPS, CHIPS)


def came_from(source):
    dx, dc = source
    core = lax.axis_index("core")
    return CORES * chip_at(-dx) + (core if dc == 0 else 1 - core)


def over_x(parts):
    out = [parts[0]]
    for part, dx in zip(parts[1:], STEPS[1:]):
        out.append(lax.ppermute(part, "x", [(i, (i + dx) % CHIPS) for i in range(CHIPS)]))
    return out


def with_partner(parts):
    return parts + [lax.ppermute(p, "core", [(0, 1), (1, 0)]) for p in parts]


def normed(values, gain_row):
    wide = values.astype(f32)
    mean_sq = jnp.mean(wide * wide, axis=-1, keepdims=True)
    return (wide * lax.rsqrt(mean_sq + epsilon) * gain_row).astype(bf16)


def prepare_kernel(chosen, ow, up, bundle, wanted, table, count):
    at = 0
    for c in range(0, ow.shape[1], LANES):
        bundle[at : at + ow.shape[0]] = ow[:, c : c + LANES]
        at += ow.shape[0]
    bundle[at:, : up.shape[2]] = up[0]
    bundle[at:, up.shape[2] :] = up[1]
    blocks = chosen.shape[0]
    owners = wanted.shape[0]
    mine = lax.axis_index(KV[0]) * lax.axis_size(KV[1]) + lax.axis_index(KV[1])
    c = chosen[...]
    valid = c >= 0
    owner = lax.shift_right_arithmetic(c, blocks.bit_length() - 1)
    local = c & (blocks - 1)
    lowest = jnp.zeros_like(c)
    lane = lax.broadcasted_iota(i32, (1, wanted.shape[2]), 1)
    for o in range(owners):
        hit = owner == o
        low = jnp.min(jnp.where(hit, local, blocks - 1), keepdims=True)
        high = jnp.max(jnp.where(hit, local, 0), keepdims=True)
        wanted[o] = jnp.where(lane == 0, low, high)
        lowest = jnp.where(hit, low, lowest)
    far = blocks + owner * PER_OWNER + jnp.where(local == lowest, 0, 1)
    table[...] = jnp.where(valid, jnp.where(owner == mine, local, far), 0)
    count[...] = jnp.broadcast_to(
        jnp.sum(jnp.where(valid, 1.0, 0.0), axis=1, keepdims=True).astype(i32), count.shape
    )


def latent_kernel(asked, lw, *refs):
    n = len(SOURCES)
    toks, (lat_out, send_out, tok, sem) = refs[:n], refs[n:]
    mine = came_from((0, 0))
    fetch = [
        pltpu.make_async_copy(part.at[:, mine], tok.at[came_from(source)], sem.at[i])
        for i, (part, source) in enumerate(zip(toks, SOURCES))
    ]
    for copy in fetch:
        copy.start()
    for copy in fetch:
        copy.wait()
    rows = lat_out.shape[0] * lat_out.shape[1]
    lhs = jnp.concatenate([tok[i].reshape(rows, tok.shape[-1]) for i in range(n)], axis=1)
    lat = jnp.dot(lhs, lw[...], preferred_element_type=f32).astype(bf16)
    lat_out[...] = lat.reshape(lat_out.shape)
    for o in range(send_out.shape[0]):
        for s in range(PER_OWNER):
            send_out[o, s] = lat_out[asked[o, 0, s]]


def pick_kernel(table, own, got, *refs):
    outs, pool = refs[:-1], refs[-1]
    blocks = own.shape[0]
    pool[:blocks] = own[...]
    pool[blocks:] = got[...]
    for out, dx in zip(outs, STEPS):
        for core in range(CORES):
            dest = CORES * chip_at(dx) + core
            for c in range(out.shape[1]):
                out[core, c] = pool[table[dest, c]]


def query_kernel(gain, qw, *refs):
    n = len(SOURCES)
    toks, outs, (tok, weights, sem) = refs[:n], refs[n:-3], refs[-3:]
    feats = toks[0].shape[1]
    fetch = [pltpu.make_async_copy(part, tok.at[i], sem.at[i]) for i, part in enumerate(toks)]
    for copy in fetch:
        copy.start()
    for i, source in enumerate(SOURCES):
        at = pl.multiple_of(came_from(source) * feats, feats)
        weights[i * feats : (i + 1) * feats] = qw[pl.ds(at, feats), :]
    for copy in fetch:
        copy.wait()
    width = gain.shape[1]
    for out, dx in zip(outs, STEPS):
        for core in range(CORES):
            dest = CORES * chip_at(dx) + core
            rows = pl.ds(pl.multiple_of(dest * BLOCK, BLOCK), BLOCK)
            lhs = jnp.concatenate([tok[i, rows, :] for i in range(n)], axis=1)
            acc = jnp.dot(lhs, weights[...], preferred_element_type=f32).astype(bf16)
            for h in range(out.shape[1]):
                out[core, h] = normed(acc[:, h * width : (h + 1) * width], gain[...])


def attend_kernel(count, kgain, ogain, *refs):
    n = len(SOURCES)
    queries, pieces, bundles = refs[:n], refs[n : 2 * n], refs[2 * n : 3 * n]
    out, q_ref, kv, weights, acc, q_sem, kv_sem, weight_sem = refs[3 * n :]
    mine = lax.axis_index("core")
    each = queries[0].shape[1]
    asked = [
        pltpu.make_async_copy(p.at[mine], q_ref.at[pl.ds(i * each, each)], q_sem.at[i])
        for i, p in enumerate(queries)
    ]
    fetch = [pltpu.make_async_copy(p.at[mine], kv.at[i], kv_sem.at[i]) for i, p in enumerate(pieces)]
    later = [
        pltpu.make_async_copy(b, weights.at[i], weight_sem.at[i]) for i, b in enumerate(bundles)
    ]
    for copy in asked + fetch + later:
        copy.start()
    for copy in asked:
        copy.wait()
    _, picks, sl, width = kv.shape
    keys = picks * sl
    heads = q_ref.shape[0]
    per = ROWS // BLOCK
    here = count[came_from((0, 0)), 0]
    gain = kgain[...] * (width**-0.5 * math.log2(math.e))
    on = lax.broadcasted_iota(i32, (keys, width), 0) < here * sl
    at = lax.broadcasted_iota(i32, (ROWS, BLOCK), 1)
    row = lax.broadcasted_iota(i32, (ROWS, BLOCK), 0) & (BLOCK - 1)
    for i, source in enumerate(SOURCES):
        fetch[i].wait()
        src = came_from(source)
        lat = kv[i].reshape(keys, width)
        lat = jnp.where(on, lat, jnp.zeros_like(lat))
        ones = jnp.where(on, jnp.ones_like(lat), jnp.zeros_like(lat))
        k = normed(lat, gain)
        v = jnp.concatenate([lat, ones], axis=1)
        for r in range(heads // per):
            q = jnp.concatenate([q_ref[r * per + h] for h in range(per)], axis=0)
            s = lax.dot_general(q, k, (((1,), (1,)), ((), ())), preferred_element_type=f32)
            w = jnp.exp2(s)
            own = jnp.where((at >= sl) | (at + src * sl <= row), w[:, :BLOCK], 0.0)
            w = jnp.concatenate([own, w[:, BLOCK:]], axis=1).astype(bf16)
            got = jnp.dot(w, v, preferred_element_type=f32)
            acc[r] = got if i == 0 else acc[r] + got
    for copy in later:
        copy.wait()
    model = ogain.shape[1]
    total = None
    for i in range(n):
        block = weights[i]
        rows = model // LANES * BLOCK
        up = jnp.concatenate([block[rows:, :width], block[rows:, width:]], axis=0)
        halves = []
        for h in (CORES * i, CORES * i + 1):
            r, k = h // per, h % per
            sums = acc[r, k * BLOCK : (k + 1) * BLOCK, :]
            att = (sums[:, :width] / sums[:, width:]).astype(bf16)
            halves.append(
                lax.dot_general(att, up, (((1,), (1,)), ((), ())), preferred_element_type=f32)
            )
        lane = lax.broadcasted_iota(i32, halves[0].shape, 1)
        side = jnp.where(lane < width // CORES, halves[0], halves[1]).astype(bf16)
        proj = jnp.concatenate(
            [block[c * BLOCK : (c + 1) * BLOCK] for c in range(model // LANES)], axis=1
        )
        part = jnp.dot(side, proj, preferred_element_type=f32)
        total = part if total is None else total + part
    mean_sq = jnp.mean(total * total, axis=-1, keepdims=True)
    res = (total * lax.rsqrt(mean_sq + epsilon) * ogain[...]).astype(bf16)
    w = out.shape[2]
    for p in range(out.shape[0]):
        out[p] = res[:, p * w : (p + 1) * w]


def shape(dims, kind=bf16):
    return jax.ShapeDtypeStruct(dims, kind)


def shards(
    tokens,
    query_weight,
    latent_weight,
    query_gain,
    key_gain,
    value_up,
    out_weight,
    out_gain,
    chosen,
):
    rows, feats = tokens.shape
    lat_w = latent_weight.shape[1]
    blocks = rows // BLOCK
    picks = chosen.shape[1]
    owners = lax.axis_size(KV)
    tp = len(SOURCES)
    sl = BLOCK // tp
    each = query_weight.shape[1] // lat_w
    heads = each * tp
    late_rows = (out_weight.size + value_up.size) // LANES

    toks_x = over_x([tokens] * CHIPS)

    bundle, wanted, table, count = pl.pallas_call(
        prepare_kernel,
        out_shape=[
            shape((late_rows, LANES)),
            shape((owners, 1, BLOCK), i32),
            shape((blocks, picks), i32),
            shape((blocks, BLOCK), i32),
        ],
        in_specs=[VMEM] * 3,
        out_specs=[VMEM] * 4,
        name="prepare",
    )(chosen, out_weight, value_up.swapaxes(1, 2))

    asked = lax.all_to_all(wanted, KV, split_axis=0, concat_axis=0, tiled=True)
    bundles_x = over_x([bundle] * CHIPS)
    toks = with_partner(toks_x)

    latent, send = pl.pallas_call(
        latent_kernel,
        out_shape=(shape((blocks, sl, lat_w)), shape((owners, PER_OWNER, sl, lat_w))),
        in_specs=[SMEM, VMEM] + [ANY] * tp,
        out_specs=(VMEM, VMEM),
        scratch_shapes=[pltpu.VMEM((tp, blocks, sl, feats), bf16), pltpu.SemaphoreType.DMA((tp,))],
        name="latent",
    )(asked, latent_weight, *[t.reshape(blocks, tp, sl, feats) for t in toks])

    got = lax.all_to_all(send, KV, split_axis=0, concat_axis=0, tiled=True)
    got = got.reshape(owners * PER_OWNER, sl, lat_w)

    queries = pl.pallas_call(
        query_kernel,
        out_shape=[shape((CORES, each, BLOCK, lat_w))] * CHIPS,
        in_specs=[VMEM, VMEM] + [ANY] * tp,
        out_specs=[VMEM] * CHIPS,
        scratch_shapes=[
            pltpu.VMEM((tp, rows, feats), bf16),
            pltpu.VMEM((tp * feats, query_weight.shape[1]), bf16),
            pltpu.SemaphoreType.DMA((tp,)),
        ],
        name="query",
    )(query_gain[None, :], query_weight, *toks)
    queries_x = over_x(queries)

    picked = pl.pallas_call(
        pick_kernel,
        out_shape=[shape((CORES, picks, sl, lat_w))] * CHIPS,
        in_specs=[SMEM, VMEM, VMEM],
        out_specs=[VMEM] * CHIPS,
        scratch_shapes=[pltpu.VMEM((blocks + owners * PER_OWNER, sl, lat_w), bf16)],
        name="pick",
    )(table, latent, got)
    picked_x = over_x(picked)
    q = with_partner(queries_x)
    bundles = with_partner(bundles_x)
    kv = with_partner(picked_x)

    width = out_weight.shape[1] // tp
    res = pl.pallas_call(
        attend_kernel,
        out_shape=shape((tp, BLOCK, width)),
        in_specs=[SMEM] + [VMEM] * 2 + [ANY] * (3 * tp),
        out_specs=VMEM,
        scratch_shapes=[
            pltpu.VMEM((heads, BLOCK, lat_w), bf16),
            pltpu.VMEM((tp, picks, sl, lat_w), bf16),
            pltpu.VMEM((tp, late_rows, LANES), bf16),
            pltpu.VMEM((heads * BLOCK // ROWS, ROWS, 2 * lat_w), f32),
            pltpu.SemaphoreType.DMA((tp,)),
            pltpu.SemaphoreType.DMA((tp,)),
            pltpu.SemaphoreType.DMA((tp,)),
        ],
        name="attend",
    )(count, key_gain[None, :], out_gain[None, :], *q, *kv, *bundles)

    res = lax.all_to_all(res, TP, split_axis=0, concat_axis=0, tiled=True)
    return res.reshape(rows, width)


def solution(mesh):
    torus = Mesh(mesh.devices.reshape(8, 4, CHIPS, CORES), ("kv_0", "kv_1", "x", "core"))
    in_specs = (
        P(KV, TP),
        P(None, TP),
        P(),
        P(),
        P(),
        P(TP, None, None),
        P(TP, None),
        P(),
        P(KV, None),
    )
    return jax.shard_map(
        shards, mesh=torus, in_specs=in_specs, out_specs=P(KV, TP), check_vma=False
    )
```
